32 devices in a mesh: sp: 8 (over z, x), tp: 4 (over y, core).
Axes of the slice: x: 2, y: 2, z: 4, core: 2. Of those that a mesh axis runs over, the one named last changes fastest.
Arguments:
- queries: bfloat16 [4096, 2048], P('sp', 'tp'), may hold values from -90 to 90, as said below
- key_rows: bfloat16 [4096, 512], P('sp', 'tp'), may hold values from -6 to 6
- value_rows: bfloat16 [4096, 512], P('sp', 'tp'), may hold values from -6 to 6
- sink_logits: float32 [16], P('tp'), may hold values from 2 to 7
- residual: bfloat16 [4096, 2048], P('sp'), may hold values from -6 to 6
- norm_gain: float32 [2048], replicated, may hold values from 0.1 to 1.9
- out_weight: bfloat16 [2048, 2048], P('tp'), may hold values from -1.5 to 1.5
- gate_weight: bfloat16 [2048, 5632], P('sp', 'tp'), may hold values from -0.125 to 0.125
- up_weight: bfloat16 [2048, 5632], P('sp', 'tp'), may hold values from -0.125 to 0.125
- down_weight: bfloat16 [5632, 2048], P('tp', 'sp'), may hold values from -0.078125 to 0.078125
Outputs:
- mixed: bfloat16 [4096, 2048], P(('sp', 'tp'))
The draws below stay inside these ranges and needn't reach their ends.
Inputs may be any that keep to these rules, and one draw needn't show every extreme that they name: queries are mostly of order one; some rows may be much larger.
All inputs are finite; a program needn't handle non-finite values.
Results may differ from the reference program's by a relative error of at most 0.012.
Values may be sent and summed in bfloat16 or wider, within the bound.
A program may use at most 128 MiB of HBM per device.

```python
import jax
import jax.numpy as jnp
from jax import lax

D = 2048
HQ = 16
HK = 4
DH = 128
FF = 5632
WIN = 128
TOKENS = 4096
N_TP = 4


def shared_draws(key):
    base = jax.random.fold_in(key, 11)
    key_query, key_keys = jax.random.split(base, 2)
    keys_wide = jnp.clip(jax.random.normal(key_keys, (TOKENS, HK * DH), jnp.float32), -5.0, 5.0)
    query_wide = jnp.clip(jax.random.normal(key_query, (TOKENS, HQ * DH), jnp.float32), -5.0, 5.0)
    return (query_wide, keys_wide)


def draw_queries(key, part):
    return shared_draws(key)[0].astype(jnp.bfloat16)


def draw_key_rows(key, part):
    return shared_draws(key)[1].astype(jnp.bfloat16)


def steps_of(stream_key, shape, cuts, smallest, largest):
    def one(position, shards_of):
        steps = jax.random.uniform(jax.random.fold_in(jax.random.fold_in(stream_key, 6), position), (shards_of,), jnp.float32, smallest / len(cuts), largest / len(cuts))
        return jnp.repeat(jnp.exp(steps), shape[position] // shards_of).reshape((-1,) + (1,) * (len(shape) - position - 1))

    factor_of = one(*cuts[0])
    for cut in cuts[1:]:
        factor_of = factor_of * one(*cut)
    return factor_of


def gaussian(stream_key, dims, spread, most, pieces=(), kind=jnp.bfloat16):
    level = steps_of(stream_key, dims, pieces, -0.22, 0.18) if pieces else 1.0
    values = jax.random.normal(stream_key, dims, jnp.float32) * spread * level
    return jnp.minimum(jnp.maximum(values, -most), most).astype(kind)


def setup_inputs(seed: int = 0) -> dict:
    key_of = jax.random.split(jax.random.key(seed), 11)
    return {
        "queries": draw_queries(jax.random.fold_in(key_of[10], 71), 0),
        "key_rows": draw_key_rows(jax.random.fold_in(key_of[10], 71), 0),
        "value_rows": gaussian(key_of[2], (TOKENS, HK * DH), 1.0, 6.0, ((0, 8), (1, 4))),
        "sink_logits": jnp.clip(2.0 + 5.0 * jax.random.uniform(key_of[3], (HQ,), jnp.float32) ** steps_of(key_of[3], (HQ,), ((0, 4),), -0.2, 0.2), 2.0, 7.0),
        "residual": gaussian(key_of[4], (TOKENS, D), 1.0, 6.0, ((0, 8),)),
        "norm_gain": jnp.clip(1.0 + 0.18 * jax.random.normal(key_of[5], (D,), jnp.float32), 0.1, 1.9),
        "out_weight": gaussian(key_of[6], (HQ * DH, D), 0.25, 1.5, ((0, 4),)),
        "gate_weight": gaussian(key_of[7], (D, FF), D ** -0.5, 0.125, ((0, 8), (1, 4))),
        "up_weight": gaussian(key_of[8], (D, FF), D ** -0.5, 0.125, ((0, 8), (1, 4))),
        "down_weight": gaussian(key_of[9], (FF, D), FF ** -0.5, 0.078125, ((0, 4), (1, 8))),
    }


EPSILON = 1e-06
MASKED = -1e+30

def attend_block(query_blk, key_blk, value_blk, sink_logits, query_pos, key_pos, seq_len):
    kv_heads = key_blk.shape[1] // DH
    group_size = query_blk.shape[1] // key_blk.shape[1]
    query_four = query_blk.reshape(query_blk.shape[0], kv_heads, group_size, DH).astype(jnp.float32)
    key_three = key_blk.reshape(key_blk.shape[0], kv_heads, DH).astype(jnp.float32)
    value_three = value_blk.reshape(value_blk.shape[0], kv_heads, DH).astype(jnp.float32)
    scores = jnp.einsum('qhgd,khd->hgqk', query_four, key_three) * DH ** (-0.5)
    allowed = (jnp.abs(key_pos[None, :] - query_pos[:, None]) <= WIN) & (key_pos[None, :] >= 0) & (key_pos[None, :] < seq_len)
    scores = jnp.where(allowed[None, None], scores, MASKED)
    sink_col = sink_logits.astype(jnp.float32).reshape(kv_heads, group_size)[:, :, None]
    highest = jnp.maximum(lax.optimization_barrier(jnp.max(scores, axis=-1)), sink_col)
    weights_exp = jnp.exp(scores - highest[..., None])
    denominator = lax.optimization_barrier(jnp.sum(weights_exp, axis=-1)) + jnp.exp(sink_col - highest)
    probabilities = (weights_exp / denominator[..., None]).astype(jnp.bfloat16)
    heads_out = jnp.einsum('hgqk,khd->qhgd', probabilities.astype(jnp.float32), value_three)
    return heads_out.astype(jnp.bfloat16).reshape(query_blk.shape[0], kv_heads * group_size * DH)

def rms_scale(rows_wide, norm_gain):
    mean_square = lax.optimization_barrier(jnp.mean(rows_wide * rows_wide, axis=-1, keepdims=True))
    return (rows_wide * lax.rsqrt(mean_square + EPSILON) * norm_gain).astype(jnp.bfloat16)

def grouped_sum(left, right, group_cols):
    result = jnp.zeros((left.shape[0], right.shape[1]), jnp.float32)
    for group_index in range(N_TP):
        lower = group_index * group_cols
        partial_term = jnp.dot(left[:, lower:lower + group_cols], right[lower:lower + group_cols], preferred_element_type=jnp.float32)
        rounded = lax.optimization_barrier(partial_term.astype(jnp.bfloat16))
        result = result + rounded.astype(jnp.float32)
    return result

def reference(queries, key_rows, value_rows, sink_logits, residual, norm_gain, out_weight, gate_weight, up_weight, down_weight):
    block_len = 2 * WIN
    key_pad = jnp.pad(key_rows, ((WIN, WIN), (0, 0)))
    value_pad = jnp.pad(value_rows, ((WIN, WIN), (0, 0)))

    def one_block(block_index):
        block_first = (block_index * block_len).astype(jnp.int32)
        query_blk = lax.dynamic_slice_in_dim(queries, block_first, block_len, 0)
        key_blk = lax.dynamic_slice_in_dim(key_pad, block_first, block_len + 2 * WIN, 0)
        value_blk = lax.dynamic_slice_in_dim(value_pad, block_first, block_len + 2 * WIN, 0)
        query_pos = block_first + jnp.arange(block_len, dtype=jnp.int32)
        key_pos = block_first - WIN + jnp.arange(block_len + 2 * WIN, dtype=jnp.int32)
        return attend_block(query_blk, key_blk, value_blk, sink_logits, query_pos, key_pos, TOKENS)
    blocks = lax.map(one_block, jnp.arange(TOKENS // block_len, dtype=jnp.int32))
    attended = blocks.reshape(TOKENS, HQ * DH)
    attn_total = grouped_sum(attended, out_weight, HQ * DH // N_TP)
    middle = residual.astype(jnp.float32) + attn_total
    normed = rms_scale(middle, norm_gain)
    gate_acc = jnp.dot(normed, gate_weight, preferred_element_type=jnp.float32)
    up_acc = jnp.dot(normed, up_weight, preferred_element_type=jnp.float32)
    hidden = (jax.nn.silu(gate_acc) * up_acc).astype(jnp.bfloat16)
    ffn_total = grouped_sum(hidden, down_weight, FF // N_TP)
    return (middle + ffn_total).astype(jnp.bfloat16)
```

```python
import functools

import jax
import jax.numpy as jnp
from jax import lax
from jax.experimental import pallas as pl
from jax.experimental.pallas import tpu as pltpu
from jax.sharding import PartitionSpec as P

DH = 128
WIN = 128


EPSILON = 1e-06
MASKED = -1e30


def with_halo(cells, sides, width):
    for axis, dim in sides:
        count = lax.axis_size(axis)
        ends = count - 1
        head = lax.slice_in_dim(cells, 0, width, axis=dim)
        tail = lax.slice_in_dim(cells, cells.shape[dim] - width, cells.shape[dim], axis=dim)
        cells = jnp.concatenate(
            [
                lax.ppermute(tail, axis, [(i, (i + 1) % count) for i in range(ends)]),
                cells,
                lax.ppermute(head, axis, [((i + 1) % count, i) for i in range(ends)]),
            ],
            axis=dim,
        )
    return cells


def attend_block(query_blk, key_blk, value_blk, sink_logits, query_pos, key_pos, seq_len):
    kv_heads = key_blk.shape[1] // DH
    group_size = query_blk.shape[1] // key_blk.shape[1]
    query_four = query_blk.reshape(query_blk.shape[0], kv_heads, group_size, DH)
    key_three = key_blk.reshape(key_blk.shape[0], kv_heads, DH)
    value_three = value_blk.reshape(value_blk.shape[0], kv_heads, DH)
    scores = jnp.einsum(
        "qhgd,khd->hgqk", query_four, key_three, preferred_element_type=jnp.float32
    ) * DH ** (-0.5)
    allowed = (
        (jnp.abs(key_pos[None, :] - query_pos[:, None]) <= WIN)
        & (key_pos[None, :] >= 0)
        & (key_pos[None, :] < seq_len)
    )
    scores = jnp.where(allowed[None, None], scores, MASKED)
    sink_col = sink_logits.reshape(kv_heads, group_size)[:, :, None]
    highest = jnp.maximum(jnp.max(scores, axis=-1), sink_col)
    weights_exp = jnp.exp(scores - highest[..., None])
    denominator = jnp.sum(weights_exp, axis=-1) + jnp.exp(sink_col - highest)
    probabilities = (weights_exp / denominator[..., None]).astype(jnp.bfloat16)
    heads_out = jnp.einsum(
        "hgqk,khd->qhgd", probabilities, value_three, preferred_element_type=jnp.float32
    )
    return heads_out.astype(jnp.bfloat16).reshape(query_blk.shape[0], kv_heads * group_size * DH)


def rms_scale(rows_wide, norm_gain):
    mean_square = jnp.mean(rows_wide * rows_wide, axis=-1, keepdims=True)
    return (rows_wide * lax.rsqrt(mean_square + EPSILON) * norm_gain).astype(jnp.bfloat16)


def fetch_down(down_weight):
    return lax.all_gather(down_weight, "sp", axis=1, tiled=True)


def shards(
    queries,
    key_rows,
    value_rows,
    sink_logits,
    residual,
    norm_gain,
    out_weight,
    gate_weight,
    up_weight,
    down_weight,
):
    tok_local = queries.shape[0]
    block_len = 2 * WIN
    share_rows = tok_local // lax.axis_size("tp")
    seq_len = tok_local * lax.axis_size("sp")
    device_offset = lax.axis_index("sp") * tok_local
    kv_pair = jnp.stack([key_rows, value_rows])
    kv_ext = with_halo(kv_pair, (("sp", 1),), WIN)

    def one_block(block_index):
        block_first = block_index * block_len
        query_blk = lax.dynamic_slice_in_dim(queries, block_first, block_len, 0)
        key_blk = lax.dynamic_slice_in_dim(kv_ext[0], block_first, block_len + 2 * WIN, 0)
        value_blk = lax.dynamic_slice_in_dim(kv_ext[1], block_first, block_len + 2 * WIN, 0)
        query_pos = device_offset + block_first + jnp.arange(block_len, dtype=jnp.int32)
        key_pos = (
            device_offset + block_first - WIN + jnp.arange(block_len + 2 * WIN, dtype=jnp.int32)
        )
        return attend_block(query_blk, key_blk, value_blk, sink_logits, query_pos, key_pos, seq_len)

    blocks = lax.map(one_block, jnp.arange(tok_local // block_len, dtype=jnp.int32))
    attended = blocks.reshape(tok_local, queries.shape[1])
    own_first = lax.axis_index("tp") * share_rows
    attn_full = lax.psum(
        jnp.dot(attended, out_weight, preferred_element_type=jnp.float32).astype(jnp.bfloat16), "tp"
    ).astype(jnp.float32)
    middle_all = residual.astype(jnp.float32) + attn_full
    normed_all = rms_scale(middle_all, norm_gain)
    middle_own = lax.dynamic_slice_in_dim(middle_all, own_first, share_rows, 0)
    gate_sectioned = lax.all_gather(gate_weight, "sp", axis=0, tiled=True)
    up_sectioned = lax.all_gather(up_weight, "sp", axis=0, tiled=True)
    gate_acc = jnp.dot(normed_all, gate_sectioned, preferred_element_type=jnp.float32)
    up_acc = jnp.dot(normed_all, up_sectioned, preferred_element_type=jnp.float32)
    down_whole = fetch_down(down_weight)
    hidden = (jax.nn.silu(gate_acc) * up_acc).astype(jnp.bfloat16)
    ffn_share = lax.psum_scatter(
        jnp.dot(hidden, down_whole, preferred_element_type=jnp.float32).astype(jnp.bfloat16),
        "tp",
        scatter_dimension=0,
        tiled=True,
    ).astype(jnp.float32)
    return (middle_own + ffn_share).astype(jnp.bfloat16)

def ring_place(index, count):
    row, side = index // 2, index % 2
    return row * (1 - side) + (count - 1 - row) * side


def ring_owner(place, count):
    side = place // (count // 2)
    row = place * (1 - side) + (count - 1 - place) * side
    return 2 * row + side


def layer_kernel(
    q_ref, k_ref, v_ref, sink_ref, gain_ref, res_ref, ow_ref, g_ref, u_ref, d_ref, out_ref,
    kx, vx, halo, ow, resid, attended, part, arecv, middle, nrm,
    gbuf, ubuf, dbuf, gacc, uacc, hidden, fpart, frecv,
    halo_s, halo_r, loc, ring_s, ring_r, attn_s, attn_r, nrm_s, nrm_r, ffn_s, ffn_r,
    *, count, tps,
):
    me = lax.axis_index("sp")
    mt = lax.axis_index("tp")
    tok = q_ref.shape[0]
    share = tok // tps
    model = ow_ref.shape[1]
    rows = g_ref.shape[0]
    cols = d_ref.shape[1]
    group = q_ref.shape[1] // k_ref.shape[1]
    kv_heads = k_ref.shape[1] // DH
    seq_len = tok * count
    full = count // 2 - 1
    opp = 2 * full
    own = opp + 1
    place = ring_place(me, count)
    fore = ring_owner((place + 1) % count, count)
    back = ring_owner((place + count - 1) % count, count)
    after = (me + 1) % count
    before = (me + count - 1) % count

    barrier = pltpu.get_barrier_semaphore()
    for target in (fore, back, after, before):
        pl.semaphore_signal(
            barrier, inc=1, device_id={"sp": target}, device_id_type=pl.DeviceIdType.MESH
        )
    for delta in range(1, tps):
        pl.semaphore_signal(
            barrier, inc=1, device_id={"tp": (mt + delta) % tps},
            device_id_type=pl.DeviceIdType.MESH,
        )
    pl.semaphore_wait(barrier, 4 + tps - 1)

    def remote(src, dst, send, recv, where):
        return pltpu.make_async_remote_copy(
            src_ref=src, dst_ref=dst, send_sem=send, recv_sem=recv,
            device_id=where, device_id_type=pl.DeviceIdType.MESH,
        )

    halos = [
        remote(k_ref.at[pl.ds(tok - WIN, WIN)], halo.at[0], halo_s.at[0], halo_r.at[0], {"sp": after}),
        remote(v_ref.at[pl.ds(tok - WIN, WIN)], halo.at[1], halo_s.at[1], halo_r.at[1], {"sp": after}),
        remote(k_ref.at[pl.ds(0, WIN)], halo.at[2], halo_s.at[2], halo_r.at[2], {"sp": before}),
        remote(v_ref.at[pl.ds(0, WIN)], halo.at[3], halo_s.at[3], halo_r.at[3], {"sp": before}),
    ]
    for copy in halos:
        copy.start()

    originals = (g_ref, u_ref, d_ref)
    stores = (gbuf, ubuf, dbuf)

    def hop(kind, way, step):
        store = stores[kind]
        slot = lambda s: way * full + s - 1
        sems = (ring_s.at[kind, way, step - 1], ring_r.at[kind, way, step - 1])
        where = {"sp": (fore, back)[way]}
        if step <= full:
            src = originals[kind] if step == 1 else store.at[slot(step - 1)]
            return remote(src, store.at[slot(step)], *sems, where)
        half = store.shape[1] // 2
        piece = pl.ds(way * half, half)
        return remote(
            store.at[slot(full), piece], store.at[opp, piece], *sems, where
        )

    def send(kind, step):
        for way in range(2):
            hop(kind, way, step).start()

    def arrive(kind, step):
        for way in range(2):
            hop(kind, way, step).wait_recv()

    for kind in range(3):
        send(kind, 1)

    locals_ = [
        pltpu.make_async_copy(ow_ref, ow, loc.at[0]),
        pltpu.make_async_copy(
            res_ref.at[pl.ds(pl.multiple_of(mt * share, share), share)], resid, loc.at[1]
        ),
        pltpu.make_async_copy(g_ref, gbuf.at[own], loc.at[2]),
        pltpu.make_async_copy(u_ref, ubuf.at[own], loc.at[3]),
        pltpu.make_async_copy(d_ref, dbuf.at[own], loc.at[4]),
    ]
    for copy in locals_:
        copy.start()

    kx[pl.ds(WIN, tok)] = k_ref[...]
    vx[pl.ds(WIN, tok)] = v_ref[...]
    for copy in halos:
        copy.wait_recv()
    kx[pl.ds(0, WIN)] = halo[0]
    vx[pl.ds(0, WIN)] = halo[1]
    kx[pl.ds(WIN + tok, WIN)] = halo[2]
    vx[pl.ds(WIN + tok, WIN)] = halo[3]
    locals_[0].wait()

    span = share + 2 * WIN
    row_at = lax.broadcasted_iota(jnp.int32, (share, span), 0)
    col_at = lax.broadcasted_iota(jnp.int32, (share, span), 1)

    def attn_send(delta):
        peer = (mt + delta) % tps
        first = pl.multiple_of(peer * share, share)
        return remote(
            part.at[pl.ds(first, share)], arecv.at[delta - 1],
            attn_s.at[delta - 1], attn_r.at[delta - 1], {"tp": peer},
        )

    def attend(delta, carry):
        first = pl.multiple_of(((mt + delta) % tps) * share, share)
        key_pos = me * tok + first - WIN + col_at
        gap = col_at - row_at
        allowed = (gap >= 0) & (gap <= 2 * WIN) & (key_pos >= 0) & (key_pos < seq_len)
        for kv in range(kv_heads):
            keys = kx[pl.ds(first, span), kv * DH:(kv + 1) * DH]
            values = vx[pl.ds(first, span), kv * DH:(kv + 1) * DH]
            for sub in range(group):
                head = kv * group + sub
                query = q_ref[pl.ds(first, share), head * DH:(head + 1) * DH]
                scores = lax.dot_general(
                    query, keys, (((1,), (1,)), ((), ())), preferred_element_type=jnp.float32
                ) * DH ** (-0.5)
                scores = jnp.where(allowed, scores, MASKED)
                sink = sink_ref[head]
                top = jnp.maximum(jnp.max(scores, axis=-1, keepdims=True), sink)
                weights = jnp.exp(scores - top)
                total = jnp.sum(weights, axis=-1, keepdims=True) + jnp.exp(sink - top)
                prob = (weights / total).astype(jnp.bfloat16)
                attended[:, head * DH:(head + 1) * DH] = jnp.dot(
                    prob, values, preferred_element_type=jnp.float32
                ).astype(jnp.bfloat16)
        part[pl.ds(first, share)] = jnp.dot(
            attended[...], ow[...], preferred_element_type=jnp.float32
        ).astype(jnp.bfloat16)

        @pl.when(delta < tps)
        def _():
            attn_send(delta).start()

        return carry

    lax.fori_loop(1, tps + 1, attend, 0)

    arrive(0, 1)
    send(0, 2)
    arrive(1, 1)
    send(1, 2)

    mine = pl.ds(pl.multiple_of(mt * share, share), share)
    locals_[1].wait()
    for delta in range(1, tps):
        attn_send(delta).wait_recv()
    strip = 32

    def norm_strip(index, carry):
        at = pl.ds(pl.multiple_of(index * strip, strip), strip)
        there = pl.ds(pl.multiple_of(mt * share + index * strip, strip), strip)
        mid = resid[at].astype(jnp.float32) + part[there].astype(jnp.float32)
        for slot in range(tps - 1):
            mid = mid + arecv[slot, at].astype(jnp.float32)
        middle[at] = mid
        mean_square = jnp.mean(mid * mid, axis=-1, keepdims=True)
        nrm[there] = (mid * lax.rsqrt(mean_square + EPSILON) * gain_ref[...]).astype(jnp.bfloat16)
        return carry

    lax.fori_loop(0, share // strip, norm_strip, 0)

    def nrm_send(delta):
        return remote(
            nrm.at[mine], nrm.at[mine],
            nrm_s.at[delta - 1], nrm_r.at[delta - 1], {"tp": (mt + delta) % tps},
        )

    def nrm_arrive(delta):
        origin = (mt + tps - delta) % tps
        there = pl.ds(pl.multiple_of(origin * share, share), share)
        return remote(
            nrm.at[there], nrm.at[there],
            nrm_s.at[delta - 1], nrm_r.at[delta - 1], {"tp": (mt + delta) % tps},
        )

    for delta in range(1, tps):
        nrm_send(delta).start()

    arrive(2, 1)
    send(2, 2)
    arrive(0, 2)
    send(0, 3)
    for delta in range(1, tps):
        nrm_arrive(delta).wait_recv()
    for copy in locals_[2:]:
        copy.wait()

    band = tok // 2

    def owner_of(slot):
        if slot == own:
            away = 0
        elif slot == opp:
            away = count // 2
        elif slot < full:
            away = count - slot - 1
        else:
            away = slot - full + 1
        return ring_owner((place + away) % count, count)

    def gate_up(slots, first):
        def one(index, carry):
            at = pl.ds(pl.multiple_of(index * band, band), band)
            for acc, store in ((gacc, gbuf), (uacc, ubuf)):
                total = None if first else acc[at]
                for slot in slots:
                    cut = pl.ds(pl.multiple_of(owner_of(slot) * rows, rows), rows)
                    term = jnp.dot(
                        nrm[at, cut], store[slot], preferred_element_type=jnp.float32
                    )
                    total = term if total is None else total + term
                acc[at] = total
            return carry

        lax.fori_loop(0, tok // band, one, 0)

    def pair(step):
        return (step - 1, full + step - 1)

    gate_up((own,), True)
    gate_up(pair(1), False)
    for step in range(2, full):
        arrive(1, step)
        send(1, step + 1)
        gate_up(pair(step), False)
        if step < full - 1:
            arrive(2, step)
            send(2, step + 1)
        arrive(0, step + 1)
        send(0, step + 2)
    arrive(1, full)
    send(1, full + 1)
    arrive(2, full - 1)
    send(2, full)
    gate_up(pair(full), False)
    arrive(0, full + 1)
    arrive(1, full + 1)
    gate_up((opp,), False)
    half_rows = 64

    def gated(index, carry):
        at = pl.ds(pl.multiple_of(index * half_rows, half_rows), half_rows)
        gate = gacc[at]
        hidden[at] = (gate / (1.0 + jnp.exp(-gate)) * uacc[at]).astype(jnp.bfloat16)
        return carry

    lax.fori_loop(0, tok // half_rows, gated, 0)

    def ffn_send(slot, delta):
        peer = (mt + delta) % tps
        first = pl.multiple_of(peer * share, share)
        return remote(
            fpart.at[slot, pl.ds(first, share)], frecv.at[slot, delta - 1],
            ffn_s.at[slot, delta - 1], ffn_r.at[slot, delta - 1], {"tp": peer},
        )

    def down(slot):
        def one(index, carry):
            at = pl.ds(pl.multiple_of(index * band, band), band)
            fpart[slot, at] = jnp.dot(
                hidden[at], dbuf[slot], preferred_element_type=jnp.float32
            ).astype(jnp.bfloat16)
            return carry

        lax.fori_loop(0, tok // band, one, 0)
        for delta in range(1, tps):
            ffn_send(slot, delta).start()

    def finish(slot):
        for delta in range(1, tps):
            ffn_send(slot, delta).wait_recv()
        cut = pl.ds(pl.multiple_of(owner_of(slot) * cols, cols), cols)
        total = middle[:, cut] + fpart[slot, mine].astype(jnp.float32)
        for other in range(tps - 1):
            total = total + frecv[slot, other].astype(jnp.float32)
        out_ref[:, cut] = total.astype(out_ref.dtype)

    down(own)
    for step in range(1, full):
        for slot in pair(step):
            down(slot)
    arrive(2, full)
    send(2, full + 1)
    for slot in pair(full):
        down(slot)
    finish(own)
    for step in range(1, full):
        for slot in pair(step):
            finish(slot)
    arrive(2, full + 1)
    down(opp)
    for slot in pair(full):
        finish(slot)
    finish(opp)

    for copy in halos:
        copy.wait_send()
    for kind in range(3):
        for step in range(1, full + 2):
            for way in range(2):
                hop(kind, way, step).wait_send()
    for delta in range(1, tps):
        attn_send(delta).wait_send()
        nrm_send(delta).wait_send()
        for slot in range(count):
            ffn_send(slot, delta).wait_send()


def fused_shards(
    queries, key_rows, value_rows, sink_logits, residual, norm_gain,
    out_weight, gate_weight, up_weight, down_weight,
):
    count, tps = lax.axis_size("sp"), lax.axis_size("tp")
    tok, model = residual.shape
    share = tok // tps
    rows, units = gate_weight.shape
    cols = down_weight.shape[1]
    full = count // 2 - 1
    kv_cols = key_rows.shape[1]
    bf, f32 = jnp.bfloat16, jnp.float32
    vmem = pl.BlockSpec(memory_space=pltpu.VMEM)
    away = pl.BlockSpec(memory_space=pl.ANY)
    dma = pltpu.SemaphoreType.DMA
    return pl.pallas_call(
        functools.partial(layer_kernel, count=count, tps=tps),
        out_shape=jax.ShapeDtypeStruct((share, model), bf),
        in_specs=[vmem, vmem, vmem, pl.BlockSpec(memory_space=pltpu.SMEM), vmem]
        + [away] * 5,
        out_specs=vmem,
        scratch_shapes=[
            pltpu.VMEM((tok + 2 * WIN, kv_cols), bf),
            pltpu.VMEM((tok + 2 * WIN, kv_cols), bf),
            pltpu.VMEM((4, WIN, kv_cols), bf),
            pltpu.VMEM(out_weight.shape, bf),
            pltpu.VMEM((share, model), bf),
            pltpu.VMEM((share, queries.shape[1]), bf),
            pltpu.VMEM((tok, model), bf),
            pltpu.VMEM((tps - 1, share, model), bf),
            pltpu.VMEM((share, model), f32),
            pltpu.VMEM((tok, model), bf),
            pltpu.VMEM((count, rows, units), bf),
            pltpu.VMEM((count, rows, units), bf),
            pltpu.VMEM((count, units, cols), bf),
            pltpu.VMEM((tok, units), f32),
            pltpu.VMEM((tok, units), f32),
            pltpu.VMEM((tok, units), bf),
            pltpu.VMEM((count, tok, cols), bf),
            pltpu.VMEM((count, tps - 1, share, cols), bf),
            dma((4,)),
            dma((4,)),
            dma((5,)),
            dma((3, 2, full + 1)),
            dma((3, 2, full + 1)),
            dma((tps - 1,)),
            dma((tps - 1,)),
            dma((tps - 1,)),
            dma((tps - 1,)),
            dma((count, tps - 1)),
            dma((count, tps - 1)),
        ],
        compiler_params=pltpu.CompilerParams(
            collective_id=0, has_side_effects=True, vmem_limit_bytes=60 * 1024 * 1024
        ),
    )(
        queries, key_rows, value_rows, sink_logits, norm_gain.reshape(1, model),
        residual, out_weight, gate_weight, up_weight, down_weight,
    )


def chosen(queries, key_rows, value_rows, sink_logits, residual, norm_gain,
           out_weight, gate_weight, up_weight, down_weight):
    count = lax.axis_size("sp")
    share = queries.shape[0] // lax.axis_size("tp")
    fits = (
        count % 2 == 0
        and 8 <= count <= 16
        and share % 128 == 0
        and gate_weight.shape[0] % 128 == 0
        and gate_weight.shape[1] % 128 == 0
        and down_weight.shape[1] % 128 == 0
    )
    return (fused_shards if fits else shards)(
        queries, key_rows, value_rows, sink_logits, residual, norm_gain,
        out_weight, gate_weight, up_weight, down_weight,
    )


def solution(mesh):
    placed = (
        P("sp", "tp"),
        P("sp", "tp"),
        P("sp", "tp"),
        P("tp"),
        P("sp", None),
        P(),
        P("tp", None),
        P("sp", "tp"),
        P("sp", "tp"),
        P("tp", "sp"),
    )
    return jax.shard_map(
        chosen, mesh=mesh, in_specs=placed, out_specs=P(("sp", "tp"), None), check_vma=False
    )
```

```python
import functools

import jax
import jax.numpy as jnp
from jax import lax
from jax.experimental import pallas as pl
from jax.experimental.pallas import tpu as pltpu
from jax.sharding import PartitionSpec as P

DH = 128
WIN = 128


EPSILON = 1e-06
MASKED = -1e30


def with_halo(cells, sides, width):
    for axis, dim in sides:
        count = lax.axis_size(axis)
        ends = count - 1
        head = lax.slice_in_dim(cells, 0, width, axis=dim)
        tail = lax.slice_in_dim(cells, cells.shape[dim] - width, cells.shape[dim], axis=dim)
        cells = jnp.concatenate(
            [
                lax.ppermute(tail, axis, [(i, (i + 1) % count) for i in range(ends)]),
                cells,
                lax.ppermute(head, axis, [((i + 1) % count, i) for i in range(ends)]),
            ],
            axis=dim,
        )
    return cells


def attend_block(query_blk, key_blk, value_blk, sink_logits, query_pos, key_pos, seq_len):
    kv_heads = key_blk.shape[1] // DH
    group_size = query_blk.shape[1] // key_blk.shape[1]
    query_four = query_blk.reshape(query_blk.shape[0], kv_heads, group_size, DH)
    key_three = key_blk.reshape(key_blk.shape[0], kv_heads, DH)
    value_three = value_blk.reshape(value_blk.shape[0], kv_heads, DH)
    scores = jnp.einsum(
        "qhgd,khd->hgqk", query_four, key_three, preferred_element_type=jnp.float32
    ) * DH ** (-0.5)
    allowed = (
        (jnp.abs(key_pos[None, :] - query_pos[:, None]) <= WIN)
        & (key_pos[None, :] >= 0)
        & (key_pos[None, :] < seq_len)
    )
    scores = jnp.where(allowed[None, None], scores, MASKED)
    sink_col = sink_logits.reshape(kv_heads, group_size)[:, :, None]
    highest = jnp.maximum(jnp.max(scores, axis=-1), sink_col)
    weights_exp = jnp.exp(scores - highest[..., None])
    denominator = jnp.sum(weights_exp, axis=-1) + jnp.exp(sink_col - highest)
    probabilities = (weights_exp / denominator[..., None]).astype(jnp.bfloat16)
    heads_out = jnp.einsum(
        "hgqk,khd->qhgd", probabilities, value_three, preferred_element_type=jnp.float32
    )
    return heads_out.astype(jnp.bfloat16).reshape(query_blk.shape[0], kv_heads * group_size * DH)


def rms_scale(rows_wide, norm_gain):
    mean_square = jnp.mean(rows_wide * rows_wide, axis=-1, keepdims=True)
    return (rows_wide * lax.rsqrt(mean_square + EPSILON) * norm_gain).astype(jnp.bfloat16)


def fetch_down(down_weight):
    return lax.all_gather(down_weight, "sp", axis=1, tiled=True)


def shards(
    queries,
    key_rows,
    value_rows,
    sink_logits,
    residual,
    norm_gain,
    out_weight,
    gate_weight,
    up_weight,
    down_weight,
):
    tok_local = queries.shape[0]
    block_len = 2 * WIN
    share_rows = tok_local // lax.axis_size("tp")
    seq_len = tok_local * lax.axis_size("sp")
    device_offset = lax.axis_index("sp") * tok_local
    kv_pair = jnp.stack([key_rows, value_rows])
    kv_ext = with_halo(kv_pair, (("sp", 1),), WIN)

    def one_block(block_index):
        block_first = block_index * block_len
        query_blk = lax.dynamic_slice_in_dim(queries, block_first, block_len, 0)
        key_blk = lax.dynamic_slice_in_dim(kv_ext[0], block_first, block_len + 2 * WIN, 0)
        value_blk = lax.dynamic_slice_in_dim(kv_ext[1], block_first, block_len + 2 * WIN, 0)
        query_pos = device_offset + block_first + jnp.arange(block_len, dtype=jnp.int32)
        key_pos = (
            device_offset + block_first - WIN + jnp.arange(block_len + 2 * WIN, dtype=jnp.int32)
        )
        return attend_block(query_blk, key_blk, value_blk, sink_logits, query_pos, key_pos, seq_len)

    blocks = lax.map(one_block, jnp.arange(tok_local // block_len, dtype=jnp.int32))
    attended = blocks.reshape(tok_local, queries.shape[1])
    own_first = lax.axis_index("tp") * share_rows
    attn_full = lax.psum(
        jnp.dot(attended, out_weight, preferred_element_type=jnp.float32).astype(jnp.bfloat16), "tp"
    ).astype(jnp.float32)
    middle_all = residual.astype(jnp.float32) + attn_full
    normed_all = rms_scale(middle_all, norm_gain)
    middle_own = lax.dynamic_slice_in_dim(middle_all, own_first, share_rows, 0)
    gate_sectioned = lax.all_gather(gate_weight, "sp", axis=0, tiled=True)
    up_sectioned = lax.all_gather(up_weight, "sp", axis=0, tiled=True)
    gate_acc = jnp.dot(normed_all, gate_sectioned, preferred_element_type=jnp.float32)
    up_acc = jnp.dot(normed_all, up_sectioned, preferred_element_type=jnp.float32)
    down_whole = fetch_down(down_weight)
    hidden = (jax.nn.silu(gate_acc) * up_acc).astype(jnp.bfloat16)
    ffn_share = lax.psum_scatter(
        jnp.dot(hidden, down_whole, preferred_element_type=jnp.float32).astype(jnp.bfloat16),
        "tp",
        scatter_dimension=0,
        tiled=True,
    ).astype(jnp.float32)
    return (middle_own + ffn_share).astype(jnp.bfloat16)

def layer_kernel(
    q_ref, k_ref, v_ref, sink_ref, gain_ref, res_ref, ow_ref, g_ref, u_ref, d_ref, out_ref,
    kx, vx, halo, ow, resid, attended, part, arecv, middle, nown, nrm,
    gbuf, ubuf, dbuf, gacc, uacc, hidden, fpart, frecv,
    halo_s, halo_r, loc, col_s, col_r, x_s, x_r, sib_s, sib_r,
    attn_s, attn_r, nrm_s, nrm_r, fwd_s, ffn_s, ffn_r,
    *, count, tps,
):
    me = lax.axis_index("sp")
    mt = lax.axis_index("tp")
    tok = q_ref.shape[0]
    share = tok // tps
    model = ow_ref.shape[1]
    rows = g_ref.shape[0]
    cols = d_ref.shape[1]
    group = q_ref.shape[1] // k_ref.shape[1]
    kv_heads = k_ref.shape[1] // DH
    seq_len = tok * count
    deep, wide = count // 2, tps // 2
    z, x, y, c = me // 2, me % 2, mt // 2, mt % 2
    p = z % 2
    turn = 1 - 2 * (z // (deep // 2))
    home_z = z - p + c
    pair_z = z + 1 - 2 * p
    after = (me + 1) % count
    before = (me + count - 1) % count

    def at_device(zz, xx, yy, cc):
        return {"sp": 2 * zz + xx, "tp": 2 * yy + cc}

    barrier = pltpu.get_barrier_semaphore()
    greeted = [{"sp": after}, {"sp": before}, {"sp": 2 * z + 1 - x}]
    for dz in range(deep):
        for dt in range(tps):
            if dz or dt:
                greeted.append({"sp": 2 * ((z + dz) % deep) + x, "tp": (mt + dt) % tps})
    for target in greeted:
        pl.semaphore_signal(
            barrier, inc=1, device_id=target, device_id_type=pl.DeviceIdType.MESH
        )
    pl.semaphore_wait(barrier, len(greeted))

    def remote(src, dst, send, recv, where):
        return pltpu.make_async_remote_copy(
            src_ref=src, dst_ref=dst, send_sem=send, recv_sem=recv,
            device_id=where, device_id_type=pl.DeviceIdType.MESH,
        )

    halos = [
        remote(k_ref.at[pl.ds(tok - WIN, WIN)], halo.at[0], halo_s.at[0], halo_r.at[0], {"sp": after}),
        remote(v_ref.at[pl.ds(tok - WIN, WIN)], halo.at[1], halo_s.at[1], halo_r.at[1], {"sp": after}),
        remote(k_ref.at[pl.ds(0, WIN)], halo.at[2], halo_s.at[2], halo_r.at[2], {"sp": before}),
        remote(v_ref.at[pl.ds(0, WIN)], halo.at[3], halo_s.at[3], halo_r.at[3], {"sp": before}),
    ]
    for copy in halos:
        copy.start()

    originals = (g_ref, u_ref, d_ref)
    stores = (gbuf, ubuf, dbuf)

    def piece(kind, owner, part_of):
        half = stores[kind].shape[1] // 2
        return stores[kind].at[owner, pl.ds(part_of * half, half)]

    def column(kind, j, h):
        half = stores[kind].shape[1] // 2
        target = 2 * ((z // 2 + j) % (deep // 2)) + c
        src = originals[kind].at[pl.ds(h * half, half)]
        dst = piece(kind, me, h)
        there = remote(
            src, dst, col_s.at[kind, j, h], col_r.at[kind, z], at_device(target, x, y, h)
        )
        here = pltpu.make_async_copy(src, dst, col_r.at[kind, z])
        return there, here, jnp.logical_and(c == p, c == h) if j == 0 else None

    def start_either(there, here, stays):
        if stays is None:
            there.start()
            return

        @pl.when(stays)
        def _():
            here.start()

        @pl.when(jnp.logical_not(stays))
        def _():
            there.start()

    def end_either(there, stays):
        if stays is None:
            there.wait_send()
            return

        @pl.when(jnp.logical_not(stays))
        def _():
            there.wait_send()

    for kind in range(3):
        for j in range(deep // 2):
            for h in range(2):
                start_either(*column(kind, j, h))

    def source_z(k):
        return (z + k * turn + deep) % deep

    def owner_of(k, side):
        return 2 * source_z(k) + (x if side == 0 else 1 - x)

    def across(kind, k):
        zs = source_z(k)
        own_piece = piece(kind, 2 * zs + x, c)
        return remote(
            own_piece, own_piece, x_s.at[kind, k], x_r.at[kind, zs], at_device(z, 1 - x, y, c)
        )

    def across_in(kind, k):
        zs = source_z(k)
        own_piece = piece(kind, 2 * zs + 1 - x, c)
        return remote(
            own_piece, own_piece, x_s.at[kind, k], x_r.at[kind, zs], at_device(z, 1 - x, y, c)
        )

    def sibling(kind, side, k, part_of):
        own_piece = piece(kind, owner_of(k, side), part_of)
        return remote(
            own_piece, own_piece, sib_s.at[kind, side, k], sib_r.at[kind, side, source_z(k)],
            at_device(z, x, y, 1 - c),
        )

    def relay(kind, k):
        zs = source_z(k)
        own_piece = piece(kind, 2 * zs + x, c)
        remote(
            own_piece, own_piece, x_s.at[kind, k], col_r.at[kind, zs], at_device(z, 1 - x, y, c)
        ).wait_recv()
        across(kind, k).start()
        sibling(kind, 0, k, c).start()

    def relay_across(kind, k):
        across_in(kind, k).wait_recv()
        sibling(kind, 1, k, c).start()

    def settle(kind, side, k):
        sibling(kind, side, k, 1 - c).wait_recv()

    locals_ = [
        pltpu.make_async_copy(ow_ref, ow, loc.at[0]),
        pltpu.make_async_copy(
            res_ref.at[pl.ds(pl.multiple_of(mt * share, share), share)], resid, loc.at[1]
        ),
    ]
    for copy in locals_:
        copy.start()
    for kind in range(3):
        relay(kind, 0)

    kx[pl.ds(WIN, tok)] = k_ref[...]
    vx[pl.ds(WIN, tok)] = v_ref[...]
    for copy in halos:
        copy.wait_recv()
    kx[pl.ds(0, WIN)] = halo[0]
    vx[pl.ds(0, WIN)] = halo[1]
    kx[pl.ds(WIN + tok, WIN)] = halo[2]
    vx[pl.ds(WIN + tok, WIN)] = halo[3]
    locals_[0].wait()

    span = share + 2 * WIN
    row_at = lax.broadcasted_iota(jnp.int32, (share, span), 0)
    col_at = lax.broadcasted_iota(jnp.int32, (share, span), 1)

    def attn_send(delta):
        peer = (mt + delta) % tps
        first = pl.multiple_of(peer * share, share)
        return remote(
            part.at[pl.ds(first, share)], arecv.at[delta - 1],
            attn_s.at[delta - 1], attn_r.at[delta - 1], {"tp": peer},
        )

    def attend(delta, carry):
        first = pl.multiple_of(((mt + delta) % tps) * share, share)
        key_pos = me * tok + first - WIN + col_at
        gap = col_at - row_at
        allowed = (gap >= 0) & (gap <= 2 * WIN) & (key_pos >= 0) & (key_pos < seq_len)
        for kv in range(kv_heads):
            keys = kx[pl.ds(first, span), kv * DH:(kv + 1) * DH]
            values = vx[pl.ds(first, span), kv * DH:(kv + 1) * DH]
            for sub in range(group):
                head = kv * group + sub
                query = q_ref[pl.ds(first, share), head * DH:(head + 1) * DH]
                scores = lax.dot_general(
                    query, keys, (((1,), (1,)), ((), ())), preferred_element_type=jnp.float32
                ) * DH ** (-0.5)
                scores = jnp.where(allowed, scores, MASKED)
                sink = sink_ref[head]
                top = jnp.maximum(jnp.max(scores, axis=-1, keepdims=True), sink)
                weights = jnp.exp(scores - top)
                total = jnp.sum(weights, axis=-1, keepdims=True) + jnp.exp(sink - top)
                prob = (weights / total).astype(jnp.bfloat16)
                attended[:, head * DH:(head + 1) * DH] = jnp.dot(
                    prob, values, preferred_element_type=jnp.float32
                ).astype(jnp.bfloat16)
        part[pl.ds(first, share)] = jnp.dot(
            attended[...], ow[...], preferred_element_type=jnp.float32
        ).astype(jnp.bfloat16)

        @pl.when(delta < tps)
        def _():
            attn_send(delta).start()

        return carry

    lax.fori_loop(1, tps + 1, attend, 0)

    for k in range(1, deep):
        relay(0, k)

    mine = pl.ds(pl.multiple_of(mt * share, share), share)
    locals_[1].wait()
    for delta in range(1, tps):
        attn_send(delta).wait_recv()
    strip = 32

    def norm_strip(index, carry):
        at = pl.ds(pl.multiple_of(index * strip, strip), strip)
        there = pl.ds(pl.multiple_of(mt * share + index * strip, strip), strip)
        mid = resid[at].astype(jnp.float32) + part[there].astype(jnp.float32)
        for slot in range(tps - 1):
            mid = mid + arecv[slot, at].astype(jnp.float32)
        middle[at] = mid
        mean_square = jnp.mean(mid * mid, axis=-1, keepdims=True)
        nown[at] = (mid * lax.rsqrt(mean_square + EPSILON) * gain_ref[...]).astype(jnp.bfloat16)
        return carry

    lax.fori_loop(0, share // strip, norm_strip, 0)

    def nrm_send(dy):
        there = remote(
            nown, nrm.at[mine], nrm_s.at[dy], nrm_r.at[mt], at_device(z, x, (y + dy) % wide, p)
        )
        here = pltpu.make_async_copy(nown, nrm.at[mine], nrm_r.at[mt])
        return there, here, c == p if dy == 0 else None

    def nrm_pair():
        return remote(
            nown, nrm.at[mine], nrm_s.at[wide], nrm_r.at[mt], at_device(pair_z, x, y, p)
        )

    def nrm_rows(dy, core):
        origin = 2 * ((y + dy) % wide) + core
        return origin, nrm.at[pl.ds(pl.multiple_of(origin * share, share), share)]

    def nrm_wait(dy, core):
        origin, block = nrm_rows(dy, core)
        pltpu.make_async_copy(block, block, nrm_r.at[origin]).wait()

    def nrm_forward(dy, core):
        origin, block = nrm_rows(0, core)
        return remote(
            block, block, fwd_s.at[dy - 1, core], nrm_r.at[origin],
            at_device(z, x, (y + dy) % wide, c),
        )

    nrm_pair().start()
    for dy in range(wide - 1, -1, -1):
        start_either(*nrm_send(dy))
    for k in range(deep):
        relay_across(0, k)
    for core in range(2):
        nrm_wait(0, core)

    @pl.when(c != p)
    def _():
        for dy in range(1, wide):
            for core in range(2):
                nrm_forward(dy, core).start()

    for k in range(1, deep):
        relay(1, k)
    for dy in range(1, wide):
        for core in range(2):
            nrm_wait(dy, core)

    band = tok // 2

    def gate_up(slots, first):
        def one(index, carry):
            at = pl.ds(pl.multiple_of(index * band, band), band)
            for acc, store in ((gacc, gbuf), (uacc, ubuf)):
                total = None if first else acc[at]
                for slot in slots:
                    cut = pl.ds(pl.multiple_of(slot * rows, rows), rows)
                    term = jnp.dot(
                        nrm[at, cut], store[slot], preferred_element_type=jnp.float32
                    )
                    total = term if total is None else total + term
                acc[at] = total
            return carry

        lax.fori_loop(0, tok // band, one, 0)

    def pair(k):
        return owner_of(k, 0), owner_of(k, 1)

    def settle_pair(k):
        for kind in range(2):
            for side in range(2):
                settle(kind, side, k)

    for k in range(deep - 1):
        relay_across(1, k)
        settle_pair(k)
        gate_up(pair(k), k == 0)
    relay_across(1, deep - 1)
    for k in range(1, deep):
        relay(2, k)
    settle_pair(deep - 1)
    gate_up(pair(deep - 1), False)
    half_rows = 64

    half_rows = 64

    def gated(index, carry):
        at = pl.ds(pl.multiple_of(index * half_rows, half_rows), half_rows)
        gate = gacc[at]
        hidden[at] = (gate / (1.0 + jnp.exp(-gate)) * uacc[at]).astype(jnp.bfloat16)
        return carry

    lax.fori_loop(0, tok // half_rows, gated, 0)

    def ffn_send(slot, delta):
        peer = (mt + delta) % tps
        block = fpart.at[slot, pl.ds(pl.multiple_of(peer * share, share), share)]
        spot = frecv.at[slot, 2 * y + p]
        there = remote(
            block, spot, ffn_s.at[slot, delta], ffn_r.at[slot, 2 * y + p],
            {"sp": 2 * home_z + x, "tp": peer},
        )
        here = pltpu.make_async_copy(block, spot, ffn_r.at[slot, 2 * y + p])
        return there, here, c == p if delta == 0 else None

    def down(slot):
        def one(index, carry):
            at = pl.ds(pl.multiple_of(index * band, band), band)
            fpart[slot, at] = jnp.dot(
                hidden[at], dbuf[slot], preferred_element_type=jnp.float32
            ).astype(jnp.bfloat16)
            return carry

        lax.fori_loop(0, tok // band, one, 0)
        for delta in range(tps):
            start_either(*ffn_send(slot, delta))

    def finish(slot):
        cut = pl.ds(pl.multiple_of(slot * cols, cols), cols)
        total = middle[:, cut]
        for other in range(tps):
            spot = frecv.at[slot, other]
            pltpu.make_async_copy(spot, spot, ffn_r.at[slot, other]).wait()
            total = total + frecv[slot, other].astype(jnp.float32)
        out_ref[:, cut] = total.astype(out_ref.dtype)

    for k in range(deep):
        settle(2, 0, k)
        down(owner_of(k, 0))
    for k in range(deep):
        relay_across(2, k)
        settle(2, 1, k)
        down(owner_of(k, 1))
    for side in range(2):
        for k in range(deep):
            finish(owner_of(k, side))

    for copy in halos:
        copy.wait_send()
    for kind in range(3):
        for j in range(deep // 2):
            for h in range(2):
                there, _, stays = column(kind, j, h)
                end_either(there, stays)
        for k in range(deep):
            across(kind, k).wait_send()
            for side in range(2):
                sibling(kind, side, k, c).wait_send()
    for delta in range(1, tps):
        attn_send(delta).wait_send()
    nrm_pair().wait_send()
    for dy in range(wide):
        there, _, stays = nrm_send(dy)
        end_either(there, stays)

    @pl.when(c != p)
    def _():
        for dy in range(1, wide):
            for core in range(2):
                nrm_forward(dy, core).wait_send()

    for slot in range(count):
        for delta in range(tps):
            there, _, stays = ffn_send(slot, delta)
            end_either(there, stays)


def fused_shards(
    queries, key_rows, value_rows, sink_logits, residual, norm_gain,
    out_weight, gate_weight, up_weight, down_weight,
):
    count, tps = lax.axis_size("sp"), lax.axis_size("tp")
    tok, model = residual.shape
    share = tok // tps
    rows, units = gate_weight.shape
    cols = down_weight.shape[1]
    deep, wide = count // 2, tps // 2
    kv_cols = key_rows.shape[1]
    bf, f32 = jnp.bfloat16, jnp.float32
    vmem = pl.BlockSpec(memory_space=pltpu.VMEM)
    away = pl.BlockSpec(memory_space=pl.ANY)
    dma = pltpu.SemaphoreType.DMA
    return pl.pallas_call(
        functools.partial(layer_kernel, count=count, tps=tps),
        out_shape=jax.ShapeDtypeStruct((share, model), bf),
        in_specs=[vmem, vmem, vmem, pl.BlockSpec(memory_space=pltpu.SMEM), vmem]
        + [away] * 5,
        out_specs=vmem,
        scratch_shapes=[
            pltpu.VMEM((tok + 2 * WIN, kv_cols), bf),
            pltpu.VMEM((tok + 2 * WIN, kv_cols), bf),
            pltpu.VMEM((4, WIN, kv_cols), bf),
            pltpu.VMEM(out_weight.shape, bf),
            pltpu.VMEM((share, model), bf),
            pltpu.VMEM((share, queries.shape[1]), bf),
            pltpu.VMEM((tok, model), bf),
            pltpu.VMEM((tps - 1, share, model), bf),
            pltpu.VMEM((share, model), f32),
            pltpu.VMEM((share, model), bf),
            pltpu.VMEM((tok, model), bf),
            pltpu.VMEM((count, rows, units), bf),
            pltpu.VMEM((count, rows, units), bf),
            pltpu.VMEM((count, units, cols), bf),
            pltpu.VMEM((tok, units), f32),
            pltpu.VMEM((tok, units), f32),
            pltpu.VMEM((tok, units), bf),
            pltpu.VMEM((count, tok, cols), bf),
            pltpu.VMEM((count, tps, share, cols), bf),
            dma((4,)),
            dma((4,)),
            dma((2,)),
            dma((3, deep // 2, 2)),
            dma((3, deep)),
            dma((3, deep)),
            dma((3, deep)),
            dma((3, 2, deep)),
            dma((3, 2, deep)),
            dma((tps - 1,)),
            dma((tps - 1,)),
            dma((wide + 1,)),
            dma((tps,)),
            dma((wide - 1, 2)),
            dma((count, tps)),
            dma((count, tps)),
        ],
        compiler_params=pltpu.CompilerParams(
            collective_id=0, has_side_effects=True, vmem_limit_bytes=60 * 1024 * 1024
        ),
    )(
        queries, key_rows, value_rows, sink_logits, norm_gain.reshape(1, model),
        residual, out_weight, gate_weight, up_weight, down_weight,
    )


def chosen(queries, key_rows, value_rows, sink_logits, residual, norm_gain,
           out_weight, gate_weight, up_weight, down_weight):
    count = lax.axis_size("sp")
    share = queries.shape[0] // lax.axis_size("tp")
    fits = (
        count % 4 == 0
        and 8 <= count <= 16
        and lax.axis_size("tp") == 4
        and share % 128 == 0
        and gate_weight.shape[0] % 128 == 0
        and gate_weight.shape[1] % 128 == 0
        and down_weight.shape[1] % 128 == 0
    )
    return (fused_shards if fits else shards)(
        queries, key_rows, value_rows, sink_logits, residual, norm_gain,
        out_weight, gate_weight, up_weight, down_weight,
    )


def solution(mesh):
    placed = (
        P("sp", "tp"),
        P("sp", "tp"),
        P("sp", "tp"),
        P("tp"),
        P("sp", None),
        P(),
        P("tp", None),
        P("sp", "tp"),
        P("sp", "tp"),
        P("tp", "sp"),
    )
    return jax.shard_map(
        chosen, mesh=mesh, in_specs=placed, out_specs=P(("sp", "tp"), None), check_vma=False
    )
```

```python
import functools

import jax
import jax.numpy as jnp
from jax import lax
from jax.experimental import pallas as pl
from jax.experimental.pallas import tpu as pltpu
from jax.sharding import PartitionSpec as P

DH = 128
WIN = 128


EPSILON = 1e-06
MASKED = -1e30


def with_halo(cells, sides, width):
    for axis, dim in sides:
        count = lax.axis_size(axis)
        ends = count - 1
        head = lax.slice_in_dim(cells, 0, width, axis=dim)
        tail = lax.slice_in_dim(cells, cells.shape[dim] - width, cells.shape[dim], axis=dim)
        cells = jnp.concatenate(
            [
                lax.ppermute(tail, axis, [(i, (i + 1) % count) for i in range(ends)]),
                cells,
                lax.ppermute(head, axis, [((i + 1) % count, i) for i in range(ends)]),
            ],
            axis=dim,
        )
    return cells


def attend_block(query_blk, key_blk, value_blk, sink_logits, query_pos, key_pos, seq_len):
    kv_heads = key_blk.shape[1] // DH
    group_size = query_blk.shape[1] // key_blk.shape[1]
    query_four = query_blk.reshape(query_blk.shape[0], kv_heads, group_size, DH)
    key_three = key_blk.reshape(key_blk.shape[0], kv_heads, DH)
    value_three = value_blk.reshape(value_blk.shape[0], kv_heads, DH)
    scores = jnp.einsum(
        "qhgd,khd->hgqk", query_four, key_three, preferred_element_type=jnp.float32
    ) * DH ** (-0.5)
    allowed = (
        (jnp.abs(key_pos[None, :] - query_pos[:, None]) <= WIN)
        & (key_pos[None, :] >= 0)
        & (key_pos[None, :] < seq_len)
    )
    scores = jnp.where(allowed[None, None], scores, MASKED)
    sink_col = sink_logits.reshape(kv_heads, group_size)[:, :, None]
    highest = jnp.maximum(jnp.max(scores, axis=-1), sink_col)
    weights_exp = jnp.exp(scores - highest[..., None])
    denominator = jnp.sum(weights_exp, axis=-1) + jnp.exp(sink_col - highest)
    probabilities = (weights_exp / denominator[..., None]).astype(jnp.bfloat16)
    heads_out = jnp.einsum(
        "hgqk,khd->qhgd", probabilities, value_three, preferred_element_type=jnp.float32
    )
    return heads_out.astype(jnp.bfloat16).reshape(query_blk.shape[0], kv_heads * group_size * DH)


def rms_scale(rows_wide, norm_gain):
    mean_square = jnp.mean(rows_wide * rows_wide, axis=-1, keepdims=True)
    return (rows_wide * lax.rsqrt(mean_square + EPSILON) * norm_gain).astype(jnp.bfloat16)


def fetch_down(down_weight):
    return lax.all_gather(down_weight, "sp", axis=1, tiled=True)


def shards(
    queries,
    key_rows,
    value_rows,
    sink_logits,
    residual,
    norm_gain,
    out_weight,
    gate_weight,
    up_weight,
    down_weight,
):
    tok_local = queries.shape[0]
    block_len = 2 * WIN
    share_rows = tok_local // lax.axis_size("tp")
    seq_len = tok_local * lax.axis_size("sp")
    device_offset = lax.axis_index("sp") * tok_local
    kv_pair = jnp.stack([key_rows, value_rows])
    kv_ext = with_halo(kv_pair, (("sp", 1),), WIN)

    def one_block(block_index):
        block_first = block_index * block_len
        query_blk = lax.dynamic_slice_in_dim(queries, block_first, block_len, 0)
        key_blk = lax.dynamic_slice_in_dim(kv_ext[0], block_first, block_len + 2 * WIN, 0)
        value_blk = lax.dynamic_slice_in_dim(kv_ext[1], block_first, block_len + 2 * WIN, 0)
        query_pos = device_offset + block_first + jnp.arange(block_len, dtype=jnp.int32)
        key_pos = (
            device_offset + block_first - WIN + jnp.arange(block_len + 2 * WIN, dtype=jnp.int32)
        )
        return attend_block(query_blk, key_blk, value_blk, sink_logits, query_pos, key_pos, seq_len)

    blocks = lax.map(one_block, jnp.arange(tok_local // block_len, dtype=jnp.int32))
    attended = blocks.reshape(tok_local, queries.shape[1])
    own_first = lax.axis_index("tp") * share_rows
    attn_full = lax.psum(
        jnp.dot(attended, out_weight, preferred_element_type=jnp.float32).astype(jnp.bfloat16), "tp"
    ).astype(jnp.float32)
    middle_all = residual.astype(jnp.float32) + attn_full
    normed_all = rms_scale(middle_all, norm_gain)
    middle_own = lax.dynamic_slice_in_dim(middle_all, own_first, share_rows, 0)
    gate_sectioned = lax.all_gather(gate_weight, "sp", axis=0, tiled=True)
    up_sectioned = lax.all_gather(up_weight, "sp", axis=0, tiled=True)
    gate_acc = jnp.dot(normed_all, gate_sectioned, preferred_element_type=jnp.float32)
    up_acc = jnp.dot(normed_all, up_sectioned, preferred_element_type=jnp.float32)
    down_whole = fetch_down(down_weight)
    hidden = (jax.nn.silu(gate_acc) * up_acc).astype(jnp.bfloat16)
    ffn_share = lax.psum_scatter(
        jnp.dot(hidden, down_whole, preferred_element_type=jnp.float32).astype(jnp.bfloat16),
        "tp",
        scatter_dimension=0,
        tiled=True,
    ).astype(jnp.float32)
    return (middle_own + ffn_share).astype(jnp.bfloat16)

def layer_kernel(
    q_ref, k_ref, v_ref, sink_ref, gain_ref, res_ref, ow_ref, g_ref, u_ref, d_ref, out_ref,
    kx, vx, halo, ow, resid, attended, part, arecv, middle, nown, nrm,
    gbuf, ubuf, dbuf, gacc, uacc, hidden, fpart, frecv,
    halo_s, halo_r, loc, col_s, col_r, x_s, x_r, sib_s, sib_r,
    attn_s, attn_r, nrm_s, nrm_r, fwd_s, ffn_s, ffn_r,
    *, count, tps,
):
    me = lax.axis_index("sp")
    mt = lax.axis_index("tp")
    tok = q_ref.shape[0]
    share = tok // tps
    model = ow_ref.shape[1]
    rows = g_ref.shape[0]
    cols = d_ref.shape[1]
    group = q_ref.shape[1] // k_ref.shape[1]
    kv_heads = k_ref.shape[1] // DH
    seq_len = tok * count
    deep, wide = count // 2, tps // 2
    z, x, y, c = me // 2, me % 2, mt // 2, mt % 2
    p = z % 2
    turn = 1 - 2 * (z // (deep // 2))
    home_z = z - p + c
    pair_z = z + 1 - 2 * p
    after = (me + 1) % count
    before = (me + count - 1) % count

    def at_device(zz, xx, yy, cc):
        return {"sp": 2 * zz + xx, "tp": 2 * yy + cc}

    barrier = pltpu.get_barrier_semaphore()
    greeted = [{"sp": after}, {"sp": before}, {"sp": 2 * z + 1 - x}]
    for dz in range(deep):
        for dt in range(tps):
            if dz or dt:
                greeted.append({"sp": 2 * ((z + dz) % deep) + x, "tp": (mt + dt) % tps})
    for target in greeted:
        pl.semaphore_signal(
            barrier, inc=1, device_id=target, device_id_type=pl.DeviceIdType.MESH
        )
    pl.semaphore_wait(barrier, len(greeted))

    def remote(src, dst, send, recv, where):
        return pltpu.make_async_remote_copy(
            src_ref=src, dst_ref=dst, send_sem=send, recv_sem=recv,
            device_id=where, device_id_type=pl.DeviceIdType.MESH,
        )

    halos = [
        remote(k_ref.at[pl.ds(tok - WIN, WIN)], halo.at[0], halo_s.at[0], halo_r.at[0], {"sp": after}),
        remote(v_ref.at[pl.ds(tok - WIN, WIN)], halo.at[1], halo_s.at[1], halo_r.at[1], {"sp": after}),
        remote(k_ref.at[pl.ds(0, WIN)], halo.at[2], halo_s.at[2], halo_r.at[2], {"sp": before}),
        remote(v_ref.at[pl.ds(0, WIN)], halo.at[3], halo_s.at[3], halo_r.at[3], {"sp": before}),
    ]
    for copy in halos:
        copy.start()

    originals = (g_ref, u_ref, d_ref)
    stores = (gbuf, ubuf, dbuf)

    def piece(kind, owner, part_of):
        half = stores[kind].shape[1] // 2
        return stores[kind].at[owner, pl.ds(part_of * half, half)]

    def column(kind, j, h):
        half = stores[kind].shape[1] // 2
        target = 2 * ((z // 2 + j) % (deep // 2)) + c
        src = originals[kind].at[pl.ds(h * half, half)]
        dst = piece(kind, me, h)
        there = remote(
            src, dst, col_s.at[kind, j, h], col_r.at[kind, z], at_device(target, x, y, h)
        )
        here = pltpu.make_async_copy(src, dst, col_r.at[kind, z])
        return there, here, jnp.logical_and(c == p, c == h) if j == 0 else None

    def start_either(there, here, stays):
        if stays is None:
            there.start()
            return

        @pl.when(stays)
        def _():
            here.start()

        @pl.when(jnp.logical_not(stays))
        def _():
            there.start()

    def end_either(there, stays):
        if stays is None:
            there.wait_send()
            return

        @pl.when(jnp.logical_not(stays))
        def _():
            there.wait_send()

    def is_late(kind, j, h):
        return kind == 2 or (kind == 1 and j > 0 and h == 1)

    def columns(late):
        for kind in range(3):
            for j in range(deep // 2):
                for h in range(2):
                    if is_late(kind, j, h) == late:
                        start_either(*column(kind, j, h))

    columns(False)

    def source_z(k):
        return (z + k * turn + deep) % deep

    def owner_of(k, side):
        return 2 * source_z(k) + (x if side == 0 else 1 - x)

    def across(kind, k):
        zs = source_z(k)
        own_piece = piece(kind, 2 * zs + x, c)
        return remote(
            own_piece, own_piece, x_s.at[kind, k], x_r.at[kind, zs], at_device(z, 1 - x, y, c)
        )

    def across_in(kind, k):
        zs = source_z(k)
        own_piece = piece(kind, 2 * zs + 1 - x, c)
        return remote(
            own_piece, own_piece, x_s.at[kind, k], x_r.at[kind, zs], at_device(z, 1 - x, y, c)
        )

    def sibling(kind, side, k, part_of):
        own_piece = piece(kind, owner_of(k, side), part_of)
        return remote(
            own_piece, own_piece, sib_s.at[kind, side, k], sib_r.at[kind, side, source_z(k)],
            at_device(z, x, y, 1 - c),
        )

    def relay(kind, k):
        zs = source_z(k)
        own_piece = piece(kind, 2 * zs + x, c)
        remote(
            own_piece, own_piece, x_s.at[kind, k], col_r.at[kind, zs], at_device(z, 1 - x, y, c)
        ).wait_recv()
        across(kind, k).start()
        sibling(kind, 0, k, c).start()

    def relay_across(kind, k):
        across_in(kind, k).wait_recv()
        sibling(kind, 1, k, c).start()

    def settle(kind, side, k):
        sibling(kind, side, k, 1 - c).wait_recv()

    locals_ = [
        pltpu.make_async_copy(ow_ref, ow, loc.at[0]),
        pltpu.make_async_copy(
            res_ref.at[pl.ds(pl.multiple_of(mt * share, share), share)], resid, loc.at[1]
        ),
    ]
    for copy in locals_:
        copy.start()
    for kind in range(2):
        relay(kind, 0)

    kx[pl.ds(WIN, tok)] = k_ref[...]
    vx[pl.ds(WIN, tok)] = v_ref[...]
    for copy in halos:
        copy.wait_recv()
    kx[pl.ds(0, WIN)] = halo[0]
    vx[pl.ds(0, WIN)] = halo[1]
    kx[pl.ds(WIN + tok, WIN)] = halo[2]
    vx[pl.ds(WIN + tok, WIN)] = halo[3]
    locals_[0].wait()

    span = share + 2 * WIN
    row_at = lax.broadcasted_iota(jnp.int32, (share, span), 0)
    col_at = lax.broadcasted_iota(jnp.int32, (share, span), 1)

    def attn_send(delta):
        peer = (mt + delta) % tps
        first = pl.multiple_of(peer * share, share)
        return remote(
            part.at[pl.ds(first, share)], arecv.at[delta - 1],
            attn_s.at[delta - 1], attn_r.at[delta - 1], {"tp": peer},
        )

    def attend(delta, carry):
        first = pl.multiple_of(((mt + delta) % tps) * share, share)
        key_pos = me * tok + first - WIN + col_at
        gap = col_at - row_at
        allowed = (gap >= 0) & (gap <= 2 * WIN) & (key_pos >= 0) & (key_pos < seq_len)
        for kv in range(kv_heads):
            keys = kx[pl.ds(first, span), kv * DH:(kv + 1) * DH]
            values = vx[pl.ds(first, span), kv * DH:(kv + 1) * DH]
            for sub in range(group):
                head = kv * group + sub
                query = q_ref[pl.ds(first, share), head * DH:(head + 1) * DH]
                scores = lax.dot_general(
                    query, keys, (((1,), (1,)), ((), ())), preferred_element_type=jnp.float32
                ) * DH ** (-0.5)
                scores = jnp.where(allowed, scores, MASKED)
                sink = sink_ref[head]
                top = jnp.maximum(jnp.max(scores, axis=-1, keepdims=True), sink)
                weights = jnp.exp(scores - top)
                total = jnp.sum(weights, axis=-1, keepdims=True) + jnp.exp(sink - top)
                prob = (weights / total).astype(jnp.bfloat16)
                attended[:, head * DH:(head + 1) * DH] = jnp.dot(
                    prob, values, preferred_element_type=jnp.float32
                ).astype(jnp.bfloat16)
        part[pl.ds(first, share)] = jnp.dot(
            attended[...], ow[...], preferred_element_type=jnp.float32
        ).astype(jnp.bfloat16)

        @pl.when(delta < tps)
        def _():
            attn_send(delta).start()

        return carry

    lax.fori_loop(1, tps + 1, attend, 0)

    for k in range(1, deep):
        relay(0, k)

    mine = pl.ds(pl.multiple_of(mt * share, share), share)
    locals_[1].wait()
    for delta in range(1, tps):
        attn_send(delta).wait_recv()
    strip = 32

    def norm_strip(index, carry):
        at = pl.ds(pl.multiple_of(index * strip, strip), strip)
        there = pl.ds(pl.multiple_of(mt * share + index * strip, strip), strip)
        mid = resid[at].astype(jnp.float32) + part[there].astype(jnp.float32)
        for slot in range(tps - 1):
            mid = mid + arecv[slot, at].astype(jnp.float32)
        middle[at] = mid
        mean_square = jnp.mean(mid * mid, axis=-1, keepdims=True)
        nown[at] = (mid * lax.rsqrt(mean_square + EPSILON) * gain_ref[...]).astype(jnp.bfloat16)
        return carry

    lax.fori_loop(0, share // strip, norm_strip, 0)

    def nrm_send(dy):
        there = remote(
            nown, nrm.at[mine], nrm_s.at[dy], nrm_r.at[mt], at_device(z, x, (y + dy) % wide, p)
        )
        here = pltpu.make_async_copy(nown, nrm.at[mine], nrm_r.at[mt])
        return there, here, c == p if dy == 0 else None

    def nrm_pair():
        return remote(
            nown, nrm.at[mine], nrm_s.at[wide], nrm_r.at[mt], at_device(pair_z, x, y, p)
        )

    def nrm_rows(dy, core):
        origin = 2 * ((y + dy) % wide) + core
        return origin, nrm.at[pl.ds(pl.multiple_of(origin * share, share), share)]

    def nrm_wait(dy, core):
        origin, block = nrm_rows(dy, core)
        pltpu.make_async_copy(block, block, nrm_r.at[origin]).wait()

    def nrm_forward(dy, core):
        origin, block = nrm_rows(0, core)
        return remote(
            block, block, fwd_s.at[dy - 1, core], nrm_r.at[origin],
            at_device(z, x, (y + dy) % wide, c),
        )

    nrm_pair().start()
    for dy in range(wide - 1, -1, -1):
        start_either(*nrm_send(dy))
    columns(True)
    for k in range(deep):
        relay_across(0, k)
    for k in range(1, deep):
        relay(1, k)
    relay(2, 0)
    for core in range(2):
        nrm_wait(0, core)

    @pl.when(c != p)
    def _():
        for dy in range(1, wide):
            for core in range(2):
                nrm_forward(dy, core).start()

    for dy in range(1, wide):
        for core in range(2):
            nrm_wait(dy, core)

    band = tok // 2

    def gate_up(slots, first):
        def one(index, carry):
            at = pl.ds(pl.multiple_of(index * band, band), band)
            for acc, store in ((gacc, gbuf), (uacc, ubuf)):
                total = None if first else acc[at]
                for slot in slots:
                    cut = pl.ds(pl.multiple_of(slot * rows, rows), rows)
                    term = jnp.dot(
                        nrm[at, cut], store[slot], preferred_element_type=jnp.float32
                    )
                    total = term if total is None else total + term
                acc[at] = total
            return carry

        lax.fori_loop(0, tok // band, one, 0)

    def pair(k):
        return owner_of(k, 0), owner_of(k, 1)

    def settle_pair(k):
        for kind in range(2):
            for side in range(2):
                settle(kind, side, k)

    for k in range(deep - 1):
        relay_across(1, k)
        settle_pair(k)
        gate_up(pair(k), k == 0)
    relay_across(1, deep - 1)
    for k in range(1, deep):
        relay(2, k)
    settle_pair(deep - 1)
    gate_up(pair(deep - 1), False)
    half_rows = 64

    half_rows = 64

    def gated(index, carry):
        at = pl.ds(pl.multiple_of(index * half_rows, half_rows), half_rows)
        gate = gacc[at]
        hidden[at] = (gate / (1.0 + jnp.exp(-gate)) * uacc[at]).astype(jnp.bfloat16)
        return carry

    lax.fori_loop(0, tok // half_rows, gated, 0)

    def ffn_send(slot, delta):
        peer = (mt + delta) % tps
        block = fpart.at[slot, pl.ds(pl.multiple_of(peer * share, share), share)]
        spot = frecv.at[slot, 2 * y + p]
        there = remote(
            block, spot, ffn_s.at[slot, delta], ffn_r.at[slot, 2 * y + p],
            {"sp": 2 * home_z + x, "tp": peer},
        )
        here = pltpu.make_async_copy(block, spot, ffn_r.at[slot, 2 * y + p])
        return there, here, c == p if delta == 0 else None

    def down(slot):
        def one(index, carry):
            at = pl.ds(pl.multiple_of(index * band, band), band)
            fpart[slot, at] = jnp.dot(
                hidden[at], dbuf[slot], preferred_element_type=jnp.float32
            ).astype(jnp.bfloat16)
            return carry

        lax.fori_loop(0, tok // band, one, 0)
        for delta in range(tps):
            start_either(*ffn_send(slot, delta))

    def finish(slot):
        cut = pl.ds(pl.multiple_of(slot * cols, cols), cols)
        total = middle[:, cut]
        for other in range(tps):
            spot = frecv.at[slot, other]
            pltpu.make_async_copy(spot, spot, ffn_r.at[slot, other]).wait()
            total = total + frecv[slot, other].astype(jnp.float32)
        out_ref[:, cut] = total.astype(out_ref.dtype)

    for k in range(deep):
        settle(2, 0, k)
        down(owner_of(k, 0))
    for k in range(deep):
        relay_across(2, k)
        settle(2, 1, k)
        down(owner_of(k, 1))
    for side in range(2):
        for k in range(deep):
            finish(owner_of(k, side))

    for copy in halos:
        copy.wait_send()
    for kind in range(3):
        for j in range(deep // 2):
            for h in range(2):
                there, _, stays = column(kind, j, h)
                end_either(there, stays)
        for k in range(deep):
            across(kind, k).wait_send()
            for side in range(2):
                sibling(kind, side, k, c).wait_send()
    for delta in range(1, tps):
        attn_send(delta).wait_send()
    nrm_pair().wait_send()
    for dy in range(wide):
        there, _, stays = nrm_send(dy)
        end_either(there, stays)

    @pl.when(c != p)
    def _():
        for dy in range(1, wide):
            for core in range(2):
                nrm_forward(dy, core).wait_send()

    for slot in range(count):
        for delta in range(tps):
            there, _, stays = ffn_send(slot, delta)
            end_either(there, stays)


def fused_shards(
    queries, key_rows, value_rows, sink_logits, residual, norm_gain,
    out_weight, gate_weight, up_weight, down_weight,
):
    count, tps = lax.axis_size("sp"), lax.axis_size("tp")
    tok, model = residual.shape
    share = tok // tps
    rows, units = gate_weight.shape
    cols = down_weight.shape[1]
    deep, wide = count // 2, tps // 2
    kv_cols = key_rows.shape[1]
    bf, f32 = jnp.bfloat16, jnp.float32
    vmem = pl.BlockSpec(memory_space=pltpu.VMEM)
    away = pl.BlockSpec(memory_space=pl.ANY)
    dma = pltpu.SemaphoreType.DMA
    return pl.pallas_call(
        functools.partial(layer_kernel, count=count, tps=tps),
        out_shape=jax.ShapeDtypeStruct((share, model), bf),
        in_specs=[vmem, vmem, vmem, pl.BlockSpec(memory_space=pltpu.SMEM), vmem]
        + [away] * 5,
        out_specs=vmem,
        scratch_shapes=[
            pltpu.VMEM((tok + 2 * WIN, kv_cols), bf),
            pltpu.VMEM((tok + 2 * WIN, kv_cols), bf),
            pltpu.VMEM((4, WIN, kv_cols), bf),
            pltpu.VMEM(out_weight.shape, bf),
            pltpu.VMEM((share, model), bf),
            pltpu.VMEM((share, queries.shape[1]), bf),
            pltpu.VMEM((tok, model), bf),
            pltpu.VMEM((tps - 1, share, model), bf),
            pltpu.VMEM((share, model), f32),
            pltpu.VMEM((share, model), bf),
            pltpu.VMEM((tok, model), bf),
            pltpu.VMEM((count, rows, units), bf),
            pltpu.VMEM((count, rows, units), bf),
            pltpu.VMEM((count, units, cols), bf),
            pltpu.VMEM((tok, units), f32),
            pltpu.VMEM((tok, units), f32),
            pltpu.VMEM((tok, units), bf),
            pltpu.VMEM((count, tok, cols), bf),
            pltpu.VMEM((count, tps, share, cols), bf),
            dma((4,)),
            dma((4,)),
            dma((2,)),
            dma((3, deep // 2, 2)),
            dma((3, deep)),
            dma((3, deep)),
            dma((3, deep)),
            dma((3, 2, deep)),
            dma((3, 2, deep)),
            dma((tps - 1,)),
            dma((tps - 1,)),
            dma((wide + 1,)),
            dma((tps,)),
            dma((wide - 1, 2)),
            dma((count, tps)),
            dma((count, tps)),
        ],
        compiler_params=pltpu.CompilerParams(
            collective_id=0, has_side_effects=True, vmem_limit_bytes=60 * 1024 * 1024
        ),
    )(
        queries, key_rows, value_rows, sink_logits, norm_gain.reshape(1, model),
        residual, out_weight, gate_weight, up_weight, down_weight,
    )


def chosen(queries, key_rows, value_rows, sink_logits, residual, norm_gain,
           out_weight, gate_weight, up_weight, down_weight):
    count = lax.axis_size("sp")
    share = queries.shape[0] // lax.axis_size("tp")
    fits = (
        count % 4 == 0
        and 8 <= count <= 16
        and lax.axis_size("tp") == 4
        and share % 128 == 0
        and gate_weight.shape[0] % 128 == 0
        and gate_weight.shape[1] % 128 == 0
        and down_weight.shape[1] % 128 == 0
    )
    return (fused_shards if fits else shards)(
        queries, key_rows, value_rows, sink_logits, residual, norm_gain,
        out_weight, gate_weight, up_weight, down_weight,
    )


def solution(mesh):
    placed = (
        P("sp", "tp"),
        P("sp", "tp"),
        P("sp", "tp"),
        P("tp"),
        P("sp", None),
        P(),
        P("tp", None),
        P("sp", "tp"),
        P("sp", "tp"),
        P("tp", "sp"),
    )
    return jax.shard_map(
        chosen, mesh=mesh, in_specs=placed, out_specs=P(("sp", "tp"), None), check_vma=False
    )
```
